32 devices in a mesh: rep: 2 (over y), fs: 4 (over z), tp: 4 (over x, core).
Axes of the slice: x: 2, y: 2, z: 4, core: 2. Of those that a mesh axis runs over, the one named last changes fastest.
Arguments:
- tokens: bfloat16 [4096, 2048], P(('rep', 'fs')), may hold values from -6 to 6
- norm_gain: float32 [2048], replicated, may hold values from 0.1 to 1.9
- gate_weight: bfloat16 [2048, 5632], P('fs', 'tp'), may hold values from -0.125 to 0.125
- up_weight: bfloat16 [2048, 5632], P('fs', 'tp'), may hold values from -0.125 to 0.125
- down_weight: bfloat16 [5632, 2048], P('tp', 'fs'), may hold values from -0.078125 to 0.078125
Outputs:
- branch_out: bfloat16 [4096, 2048], P(('rep', 'fs'))
The draws below stay inside these ranges and needn't reach their ends.
All inputs are finite; a program needn't handle non-finite values.
Results may differ from the reference program's by a relative error of at most 0.014.
Values may be sent and summed in bfloat16 or wider, within the bound.
A program may use at most 64 MiB of HBM per device.

```python
import jax
import jax.numpy as jnp
from jax import lax

D = 2048
FF = 5632
TOKENS = 4096
N_TP = 4


def steps_of(key, shape, cuts, low, top_value):
    def one(axis_at, blocks):
        steps = jax.random.uniform(jax.random.fold_in(jax.random.fold_in(key, 6), axis_at), (blocks,), jnp.float32, low / len(cuts), top_value / len(cuts))
        return jnp.repeat(jnp.exp(steps), shape[axis_at] // blocks).reshape((-1,) + (1,) * (len(shape) - axis_at - 1))

    level = one(*cuts[0])
    for cut in cuts[1:]:
        level = level * one(*cut)
    return level


def gaussian(rng, shape, scale, most, split=(), kind=jnp.bfloat16):
    drawn = scale * jax.random.normal(rng, shape, jnp.float32)
    if split:
        drawn = drawn * steps_of(rng, shape, split, -0.22, 0.18)
    return jnp.clip(drawn, -most, most).astype(kind)


def setup_inputs(seed: int = 0) -> dict:
    streams_of = jax.random.split(jax.random.key(seed), 6)
    return {
        "tokens": gaussian(streams_of[0], (TOKENS, D), 1.0, 6.0, ((0, 8),)),
        "norm_gain": jnp.clip(1.0 + 0.18 * jax.random.normal(streams_of[1], (D,), jnp.float32), 0.1, 1.9),
        "gate_weight": gaussian(streams_of[2], (D, FF), D ** -0.5, 0.125, ((0, 4), (1, 4))),
        "up_weight": gaussian(streams_of[3], (D, FF), D ** -0.5, 0.125, ((0, 4), (1, 4))),
        "down_weight": gaussian(streams_of[4], (FF, D), FF ** -0.5, 0.078125, ((0, 4), (1, 4))),
    }


def reference(tokens, norm_gain, gate_weight, up_weight, down_weight):
    wide_tok = tokens.astype(jnp.float32)
    scale = jax.lax.rsqrt(lax.optimization_barrier(jnp.mean(wide_tok * wide_tok, axis=-1, keepdims=True)) + 1e-06)
    normed = (wide_tok * scale * norm_gain).astype(jnp.bfloat16)
    gate = jnp.dot(normed, gate_weight, preferred_element_type=jnp.float32)
    up = jnp.dot(normed, up_weight, preferred_element_type=jnp.float32)
    hidden = (jax.nn.silu(gate) * up).astype(jnp.bfloat16)
    width = FF // N_TP
    total = jnp.zeros((hidden.shape[0], D), jnp.float32)
    for block in range(N_TP):
        partial_value = jnp.dot(hidden[:, block * width:(block + 1) * width], down_weight[block * width:(block + 1) * width], preferred_element_type=jnp.float32).astype(jnp.bfloat16)
        total = total + partial_value.astype(jnp.float32)
    return total.astype(jnp.bfloat16)
```

```python
import functools

import jax
import jax.numpy as jnp
from jax import lax
from jax.experimental import pallas as pl
from jax.experimental.pallas import tpu as pltpu
from jax.sharding import PartitionSpec as P

MESH = pl.DeviceIdType.MESH
F32 = jnp.float32
BF16 = jnp.bfloat16


def plain(tokens, norm_gain, gate_weight, up_weight, down_weight):
    wide_tok = tokens.astype(F32)
    scale = lax.rsqrt(jnp.mean(wide_tok * wide_tok, axis=-1, keepdims=True) + 1e-06)
    normed = (wide_tok * scale * norm_gain).astype(BF16)
    gate = jnp.dot(normed, lax.all_gather(gate_weight, "fs", axis=0, tiled=True), preferred_element_type=F32)
    up = jnp.dot(normed, lax.all_gather(up_weight, "fs", axis=0, tiled=True), preferred_element_type=F32)
    hidden = (jax.nn.silu(gate) * up).astype(BF16)
    down = lax.all_gather(down_weight, "fs", axis=1, tiled=True)
    partial_value = jnp.dot(hidden, down, preferred_element_type=F32)
    return lax.psum(partial_value.astype(BF16), "tp")


CHUNKS = 2
LAG = 2


def kernel(
    n, tok_ref, gain_ref, wg_ref, wu_ref, wd_ref, out_ref,
    normed, bg, bu, bd, gate, up, hidden, part, r1, sbuf, r2, outv,
    loc_sem, zsend, zrecv, ysend, yrecv, psend, precv, xsend, xrecv, qsend, qrecv, osem,
):
    z = lax.axis_index("fs")
    y = lax.axis_index("rep")
    t = lax.axis_index("tp")
    c = lax.rem(t, 2)
    tokens, width = tok_ref.shape
    depth, units = wg_ref.shape
    cols = wd_ref.shape[1] // CHUNKS
    half_k, half_u, half_t = depth // 2, units // 2, tokens // 2
    mate = {"tp": t + 1 - 2 * c}
    across = {"tp": lax.rem(t + 2, 4)}
    peer = {"rep": 1 - y}

    barrier = pltpu.get_barrier_semaphore()

    around = ({"fs": lax.rem(z + 1, n)}, {"fs": lax.rem(z + n - 1, n)})
    for one in around + (mate, across, peer):
        pl.semaphore_signal(barrier, 1, device_id=one, device_id_type=MESH)
    pl.semaphore_wait(barrier, 5)

    def rows_of(u, who):
        size = half_k if u < 2 else half_u
        return pl.ds(pl.multiple_of(who * size, size), size)

    def slot(u, blk, who):
        if u == 0:
            return bg.at[blk, rows_of(u, who)]
        if u == 1:
            return bu.at[blk, rows_of(u, who)]
        return bd.at[blk, u - 2, rows_of(u, who)]

    def own(u):
        if u == 0:
            return wg_ref.at[rows_of(u, y)]
        if u == 1:
            return wu_ref.at[rows_of(u, y)]
        return wd_ref.at[rows_of(u, y), pl.ds((u - 2) * cols, cols)]

    def along(u, blk, way, src=None):
        return pltpu.make_async_remote_copy(
            src_ref=slot(u, blk, y) if src is None else src,
            dst_ref=slot(u, blk, y),
            send_sem=zsend.at[u, blk, way],
            recv_sem=zrecv.at[u, blk],
            device_id={"fs": z - 1 + 2 * way},
            device_id_type=MESH,
        )

    def swap(u, blk, who):
        return pltpu.make_async_remote_copy(
            src_ref=slot(u, blk, who),
            dst_ref=slot(u, blk, who),
            send_sem=ysend.at[u, blk],
            recv_sem=yrecv.at[u, blk],
            device_id=peer,
            device_id_type=MESH,
        )

    def send_own(units_now, way):
        for u in units_now:
            along(u, z, way, own(u)).start()

    D_UNITS = tuple(range(2, 2 + CHUNKS))
    pl.when(z > 0)(lambda: send_own((0, 1), 0))
    pl.when(z < n - 1)(lambda: send_own((0, 1), 1))
    pl.when(z == n - 1)(lambda: send_own(D_UNITS, 0))
    pl.when(z == 0)(lambda: send_own(D_UNITS, 1))

    locals_ = [
        pltpu.make_async_copy(wg_ref, bg.at[z], loc_sem.at[0]),
        pltpu.make_async_copy(wu_ref, bu.at[z], loc_sem.at[1]),
    ] + [
        pltpu.make_async_copy(wd_ref.at[:, pl.ds(j * cols, cols)], bd.at[z, j], loc_sem.at[2 + j])
        for j in range(CHUNKS)
    ]
    for copy in locals_:
        copy.start()

    step = 64

    @pl.loop(0, tokens // step)
    def _(i):
        at = pl.ds(pl.multiple_of(i * step, step), step)
        wide = tok_ref[at, :].astype(F32)
        scale = lax.rsqrt(jnp.mean(wide * wide, axis=-1, keepdims=True) + 1e-06)
        normed[at, :] = (wide * scale * gain_ref[...]).astype(BF16)

    def add_dot(u, blk, first=False):
        total, held = (gate, bg) if u == 0 else (up, bu)

        @pl.loop(0, 2)
        def _(i):
            at = pl.ds(pl.multiple_of(i * half_t, half_t), half_t)
            left = normed[at, pl.ds(pl.multiple_of(blk * depth, depth), depth)]
            value = jnp.dot(left, held[blk], preferred_element_type=F32)
            total[at, :] = value if first else total[at, :] + value

    def place(blk, j, who):
        return (
            pl.ds(pl.multiple_of(who * half_t, half_t), half_t),
            pl.ds(pl.multiple_of(blk * (cols * CHUNKS) + j * cols, cols), cols),
        )

    def to_mate(blk, j):
        return pltpu.make_async_remote_copy(
            part.at[blk, j, 1], r1.at[blk, j], psend.at[blk, j], precv.at[blk, j],
            device_id=mate, device_id_type=MESH)

    def to_across(blk, j):
        return pltpu.make_async_remote_copy(
            sbuf.at[blk, j], r2.at[blk, j], xsend.at[blk, j], xrecv.at[blk, j],
            device_id=across, device_id_type=MESH)

    def give(blk, j, who):
        return pltpu.make_async_remote_copy(
            outv.at[place(blk, j, who)], outv.at[place(blk, j, who)], qsend.at[blk, j], qrecv.at[blk, j],
            device_id=mate, device_id_type=MESH)

    def write(blk, j):
        at = pl.ds(pl.multiple_of(blk * (cols * CHUNKS) + j * cols, cols), cols)
        return pltpu.make_async_copy(outv.at[:, at], out_ref.at[:, at], osem.at[blk, j])

    def make_part(blk, j):
        @pl.loop(0, 2)
        def _(i):
            side = 1 - i
            whose = c + side - 2 * c * side
            at = pl.ds(pl.multiple_of(whose * half_t, half_t), half_t)
            value = jnp.dot(hidden[at, :], bd[blk, j], preferred_element_type=F32)
            part[blk, j, side] = value.astype(BF16)

        to_mate(blk, j).start()

    def add_pair(blk, j):
        to_mate(blk, j).wait_recv()
        sbuf[blk, j] = (part[blk, j, 0].astype(F32) + r1[blk, j].astype(F32)).astype(BF16)
        to_across(blk, j).start()

    def finish(blk, j):
        to_across(blk, j).wait_recv()
        outv[place(blk, j, c)] = (sbuf[blk, j].astype(F32) + r2[blk, j].astype(F32)).astype(BF16)
        give(blk, j, c).start()

    def store(blk, j):
        give(blk, j, 1 - c).wait_recv()
        write(blk, j).start()

    def sides(k, body):
        @pl.loop(0, 2)
        def _(way):
            blk = z + k - 2 * k * way

            @pl.when(jnp.logical_and(blk >= 0, blk < n))
            def _():
                body(blk, way)

    def forward(u, k):
        def body(blk, way):
            along(u, blk, way).wait_recv()

            @pl.when(jnp.logical_or(jnp.logical_and(way == 0, z > 0), jnp.logical_and(way == 1, z < n - 1)))
            def _():
                along(u, blk, way).start()

            swap(u, blk, y).start()

        sides(k, body)

    def both(body, blk, j):
        body(blk, j)

    behind = []

    def use(u, k):
        if u < 2:
            def body(blk, way):
                swap(u, blk, 1 - y).wait_recv()
                add_dot(u, blk)

            sides(k, body)
            return

        def body(blk, way):
            swap(u, blk, 1 - y).wait_recv()
            make_part(blk, u - 2)

        sides(k, body)
        advance(k, u - 2)

    def advance(k, j):
        if behind:
            old = behind.pop()
            run(old[0], lambda blk: finish(blk, old[1]))
            late.append(old)
        run(k, lambda blk: add_pair(blk, j))
        if late:
            old = late.pop()
            run(old[0], lambda blk: store(blk, old[1]))
        behind.append((k, j))

    late = []

    def run(k, body):
        if k == 0:
            body(z)
        else:
            sides(k, lambda blk, way: body(blk))

    def middle():
        @pl.loop(0, tokens // step)
        def _(i):
            at = pl.ds(pl.multiple_of(i * step, step), step)
            value = gate[at, :]
            hidden[at, :] = (value / (1.0 + jnp.exp(-value)) * up[at, :]).astype(BF16)

        for j in range(CHUNKS):
            locals_[2 + j].wait()
            make_part(z, j)
            advance(0, j)

    for u in (0, 1):
        locals_[u].wait()
        add_dot(u, z, first=True)

    events = [(u, k) for k in range(1, n) for u in (0, 1)]
    last_row = len(events)
    events += [(u, k) for k in range(1, n) for u in D_UNITS]
    for i in range(len(events) + LAG):
        if i < len(events):
            u, k = events[i]
            forward(u, k)
            if u == 1:
                pl.when(jnp.logical_and(n - 1 - z == k, z > 0))(lambda: send_own(D_UNITS, 0))
                pl.when(jnp.logical_and(z == k, z < n - 1))(lambda: send_own(D_UNITS, 1))
        if i >= LAG:
            use(*events[i - LAG])
            if i - LAG == last_row - 1:
                middle()
    k, j = behind.pop()
    run(k, lambda blk: finish(blk, j))
    run(k, lambda blk: store(blk, j))

    for u in range(2 + CHUNKS):
        pl.when(z > 0)(lambda: along(u, z, 0, own(u)).wait_send())
        pl.when(z < n - 1)(lambda: along(u, z, 1, own(u)).wait_send())
        for k in range(1, n):
            def sent(blk, way):
                @pl.when(jnp.logical_or(jnp.logical_and(way == 0, z > 0), jnp.logical_and(way == 1, z < n - 1)))
                def _():
                    along(u, blk, way).wait_send()

                swap(u, blk, y).wait_send()

            sides(k, sent)

    @pl.loop(0, n)
    def _(blk):
        for j in range(CHUNKS):
            to_mate(blk, j).wait_send()
            to_across(blk, j).wait_send()
            give(blk, j, c).wait_send()
            write(blk, j).wait()


def fused(n, tokens, norm_gain, gate_weight, up_weight, down_weight):
    rows, width = tokens.shape
    depth, units = gate_weight.shape
    cols = down_weight.shape[1] // CHUNKS
    dma = pltpu.SemaphoreType.DMA
    grid_of = (n, CHUNKS)
    hbm = pl.BlockSpec(memory_space=pl.ANY)
    vmem = pl.BlockSpec(memory_space=pltpu.VMEM)
    return pl.pallas_call(
        functools.partial(kernel, n),
        out_shape=jax.ShapeDtypeStruct((rows, width), BF16),
        in_specs=[vmem, vmem, hbm, hbm, hbm],
        out_specs=hbm,
        scratch_shapes=[
            pltpu.VMEM((rows, width), BF16),
            pltpu.VMEM((n, depth, units), BF16),
            pltpu.VMEM((n, depth, units), BF16),
            pltpu.VMEM((n, CHUNKS, units, cols), BF16),
            pltpu.VMEM((rows, units), F32),
            pltpu.VMEM((rows, units), F32),
            pltpu.VMEM((rows, units), BF16),
            pltpu.VMEM((n, CHUNKS, 2, rows // 2, cols), BF16),
            pltpu.VMEM((n, CHUNKS, rows // 2, cols), BF16),
            pltpu.VMEM((n, CHUNKS, rows // 2, cols), BF16),
            pltpu.VMEM((n, CHUNKS, rows // 2, cols), BF16),
            pltpu.VMEM((rows, width), BF16),
            dma((2 + CHUNKS,)),
            dma((2 + CHUNKS, n, 2)),
            dma((2 + CHUNKS, n)),
            dma((2 + CHUNKS, n)),
            dma((2 + CHUNKS, n)),
        ] + [dma(grid_of) for _ in range(7)],
        compiler_params=pltpu.CompilerParams(
            collective_id=0, has_side_effects=True, vmem_limit_bytes=60 * 2**20
        ),
    )(tokens, norm_gain.reshape(1, width), gate_weight, up_weight, down_weight)


def solution(mesh):
    n = mesh.shape["fs"]
    small = mesh.shape["rep"] == 2 and mesh.shape["tp"] == 4 and n <= 4
    body = functools.partial(fused, n) if small else plain
    in_specs = (P(("rep", "fs"), None), P(), P("fs", "tp"), P("fs", "tp"), P("tp", "fs"))
    out_specs = P(("rep", "fs"), None)
    return jax.shard_map(
        body, mesh=mesh, in_specs=in_specs, out_specs=out_specs, check_vma=False
    )
```

```python
import functools

import jax
import jax.numpy as jnp
from jax import lax
from jax.experimental import pallas as pl
from jax.experimental.pallas import tpu as pltpu
from jax.sharding import PartitionSpec as P

MESH = pl.DeviceIdType.MESH
F32 = jnp.float32
BF16 = jnp.bfloat16


def plain(tokens, norm_gain, gate_weight, up_weight, down_weight):
    wide_tok = tokens.astype(F32)
    scale = lax.rsqrt(jnp.mean(wide_tok * wide_tok, axis=-1, keepdims=True) + 1e-06)
    normed = (wide_tok * scale * norm_gain).astype(BF16)
    gate = jnp.dot(normed, lax.all_gather(gate_weight, "fs", axis=0, tiled=True), preferred_element_type=F32)
    up = jnp.dot(normed, lax.all_gather(up_weight, "fs", axis=0, tiled=True), preferred_element_type=F32)
    hidden = (jax.nn.silu(gate) * up).astype(BF16)
    down = lax.all_gather(down_weight, "fs", axis=1, tiled=True)
    partial_value = jnp.dot(hidden, down, preferred_element_type=F32)
    return lax.psum(partial_value.astype(BF16), "tp")


CHUNKS = 2
LAG = 2


def kernel(
    n, tok_ref, gain_ref, wg_ref, wu_ref, wd_ref, out_ref,
    tokp, normed, bg, bu, bd, gate, up, hidden, part, r1, sbuf, rz, sx, r2, outv,
    loc_sem, zsend, zrecv, ysend, yrecv, tsend, trecv,
    psend, precv, wsend, wrecv, xsend, xrecv, qsend, qrecv, osem,
):
    z = lax.axis_index("fs")
    y = lax.axis_index("rep")
    t = lax.axis_index("tp")
    c = lax.rem(t, 2)
    tokens, width = tok_ref.shape
    depth, units = wg_ref.shape
    cols = wd_ref.shape[1] // CHUNKS
    half_k, half_t, quarter = depth // 2, tokens // 2, tokens // 4
    mid = 128
    most = (units - mid) // 2
    e = lax.rem(z, 2)
    low = z - e
    pair = {"fs": z + 1 - 2 * e}
    has_mid = e == c
    parts = ((0, most, 0), (most, mid, c), (most + mid, most, 1))
    mine = pl.multiple_of(e * (most + mid), mid)
    spans = ((mine, most), (most, mid))
    mate = {"tp": t + 1 - 2 * c}
    across = {"tp": lax.rem(t + 2, 4)}
    peer = {"rep": 1 - y}

    barrier = pltpu.get_barrier_semaphore()

    around = ({"fs": lax.rem(z + 1, n)}, {"fs": lax.rem(z + n - 1, n)})
    others = tuple({"tp": lax.rem(t + d, 4)} for d in (1, 2, 3))
    for one in around + others + (peer,):
        pl.semaphore_signal(barrier, 1, device_id=one, device_id_type=MESH)
    pl.semaphore_wait(barrier, 6)

    def token_move(quart, to, sem, first):
        at = pl.ds(pl.multiple_of(quart * quarter, quarter), quarter)
        return pltpu.make_async_remote_copy(
            src_ref=(tok_ref if first else tokp).at[at],
            dst_ref=tokp.at[at],
            send_sem=tsend.at[sem],
            recv_sem=trecv.at[quart],
            device_id=to,
            device_id_type=MESH,
        )

    token_move(t, pair, 0, True).start()

    def window(u, span, who):
        start, size = span
        if u < 2:
            return (pl.ds(pl.multiple_of(who * half_k, half_k), half_k), pl.ds(start, size))
        row = start + who * (size // 2)
        return (pl.ds(pl.multiple_of(row, 64), size // 2),)

    def slot(u, blk, span, who):
        if u < 2:
            return (bg, bu)[u].at[(blk,) + window(u, span, who)]
        return bd.at[(blk, u - 2) + window(u, span, who)]

    def own(u, span):
        if u < 2:
            return (wg_ref, wu_ref)[u].at[window(u, span, y)]
        return wd_ref.at[window(u, span, y) + (pl.ds((u - 2) * cols, cols),)]

    def along(u, blk, p, way, first=False):
        span = parts[p][:2]
        return pltpu.make_async_remote_copy(
            src_ref=own(u, span) if first else slot(u, blk, span, y),
            dst_ref=slot(u, blk, span, y),
            send_sem=zsend.at[u, blk, p, way],
            recv_sem=zrecv.at[u, blk, p],
            device_id={"fs": z - 1 + 2 * way},
            device_id_type=MESH,
        )

    def passes(p, way):
        q = parts[p][2]
        return jnp.logical_or(
            jnp.logical_and(way == 0, z > q), jnp.logical_and(way == 1, z < n - 2 + q))

    def arrives(p, way):
        q = parts[p][2]
        return jnp.logical_or(
            jnp.logical_and(way == 0, z >= q), jnp.logical_and(way == 1, z < n - 1 + q))

    def swap(u, blk, i, who):
        return pltpu.make_async_remote_copy(
            src_ref=slot(u, blk, spans[i], who),
            dst_ref=slot(u, blk, spans[i], who),
            send_sem=ysend.at[u, blk, i],
            recv_sem=yrecv.at[u, blk, i],
            device_id=peer,
            device_id_type=MESH,
        )

    def send_own(units_now, way):
        for u in units_now:
            for p in range(3):
                pl.when(passes(p, jnp.int32(way)))(lambda: along(u, z, p, way, True).start())

    D_UNITS = tuple(range(2, 2 + CHUNKS))
    send_own((0, 1), 0)
    send_own((0, 1), 1)
    pl.when(z == n - 1)(lambda: send_own(D_UNITS, 0))
    pl.when(z == 0)(lambda: send_own(D_UNITS, 1))

    locals_ = [
        pltpu.make_async_copy(wg_ref, bg.at[z], loc_sem.at[0]),
        pltpu.make_async_copy(wu_ref, bu.at[z], loc_sem.at[1]),
    ] + [
        pltpu.make_async_copy(wd_ref.at[:, pl.ds(j * cols, cols)], bd.at[z, j], loc_sem.at[2 + j])
        for j in range(CHUNKS)
    ]
    for copy in locals_:
        copy.start()

    step = 64

    def norm(src, base):
        @pl.loop(0, tokens // step)
        def _(i):
            at = pl.ds(pl.multiple_of(i * step, step), step)
            to = pl.ds(pl.multiple_of(base + i * step, step), step)
            wide = src[at, :].astype(F32)
            scale = lax.rsqrt(jnp.mean(wide * wide, axis=-1, keepdims=True) + 1e-06)
            normed[to, :] = (wide * scale * gain_ref[...]).astype(BF16)

    norm(tok_ref, 0)

    def add_dot(u, blk, first=False):
        total, held = (gate, bg) if u == 0 else (up, bu)

        def piece(start, size, base):
            @pl.loop(0, 4)
            def _(i):
                at = pl.ds(pl.multiple_of(i * half_t, half_t), half_t)
                left = normed[at, pl.ds(pl.multiple_of(blk * depth, depth), depth)]
                value = jnp.dot(left, held[blk, :, pl.ds(start, size)], preferred_element_type=F32)
                to = pl.ds(base, size)
                total[at, to] = value if first else total[at, to] + value

        piece(mine, most, 0)
        pl.when(has_mid)(lambda: piece(most, mid, most))

    def place(blk, j, who):
        return (
            pl.ds(pl.multiple_of(who * half_t, half_t), half_t),
            pl.ds(pl.multiple_of(blk * (cols * CHUNKS) + j * cols, cols), cols),
        )

    def to_mate(blk, j):
        return pltpu.make_async_remote_copy(
            part.at[blk, j, 1], r1.at[blk, j], psend.at[blk, j], precv.at[blk, j],
            device_id=mate, device_id_type=MESH)

    def to_across(blk, j):
        return pltpu.make_async_remote_copy(
            sx.at[blk, j], r2.at[blk, j], xsend.at[blk, j], xrecv.at[blk, j],
            device_id=across, device_id_type=MESH)

    def give(blk, j, who):
        return pltpu.make_async_remote_copy(
            outv.at[place(blk, j, who)], outv.at[place(blk, j, who)], qsend.at[blk, j], qrecv.at[blk, j],
            device_id=mate, device_id_type=MESH)

    def write(blk, j):
        at = pl.ds(pl.multiple_of(blk * (cols * CHUNKS) + j * cols, cols), cols)
        return pltpu.make_async_copy(outv.at[:, at], out_ref.at[:, at], osem.at[blk, j])

    def to_pair(blk, j):
        return pltpu.make_async_remote_copy(
            sbuf.at[blk, j, 1], rz.at[blk, j], wsend.at[blk, j], wrecv.at[blk, j],
            device_id=pair, device_id_type=MESH)

    def make_part(blk, j):
        def fill(with_mid):
            @pl.loop(0, 4)
            def _(i):
                side, which = i // 2, lax.rem(i, 2)
                whose = c + side - 2 * c * side
                at = pl.ds(pl.multiple_of(which * tokens + whose * half_t, half_t), half_t)
                value = jnp.dot(
                    hidden[at, pl.ds(0, most)], bd[blk, j, pl.ds(mine, most), :], preferred_element_type=F32)
                if with_mid:
                    value = value + jnp.dot(
                        hidden[at, pl.ds(most, mid)], bd[blk, j, pl.ds(most, mid), :], preferred_element_type=F32)
                part[blk, j, side, which] = value.astype(BF16)

        pl.when(has_mid)(lambda: fill(True))
        pl.when(jnp.logical_not(has_mid))(lambda: fill(False))
        to_mate(blk, j).start()

    def add_pair(blk, j):
        to_mate(blk, j).wait_recv()
        sbuf[blk, j] = (part[blk, j, 0].astype(F32) + r1[blk, j].astype(F32)).astype(BF16)
        to_pair(blk, j).start()

    def add_line(blk, j):
        to_pair(blk, j).wait_recv()
        sx[blk, j] = (sbuf[blk, j, 0].astype(F32) + rz[blk, j].astype(F32)).astype(BF16)
        to_across(blk, j).start()

    def finish(blk, j):
        to_across(blk, j).wait_recv()
        outv[place(blk, j, c)] = (sx[blk, j].astype(F32) + r2[blk, j].astype(F32)).astype(BF16)
        give(blk, j, c).start()

    def store(blk, j):
        give(blk, j, 1 - c).wait_recv()
        write(blk, j).start()

    def sides(k, body):
        @pl.loop(0, 2)
        def _(way):
            blk = z + k - 2 * k * way

            @pl.when(jnp.logical_and(blk >= 0, blk < n))
            def _():
                body(blk, way)

    def forward(u, k):
        def body(blk, way):
            for p in range(3):
                @pl.when(arrives(p, way))
                def _():
                    along(u, blk, p, way).wait_recv()
                    pl.when(passes(p, way))(lambda: along(u, blk, p, way).start())

            swap(u, blk, 0, y).start()
            pl.when(has_mid)(lambda: swap(u, blk, 1, y).start())

        sides(k, body)

    def use(u, k):
        def body(blk, way):
            swap(u, blk, 0, 1 - y).wait_recv()
            pl.when(has_mid)(lambda: swap(u, blk, 1, 1 - y).wait_recv())
            if u < 2:
                add_dot(u, blk)
            else:
                make_part(blk, u - 2)

        sides(k, body)
        if u >= 2:
            advance(k, u - 2)

    def reached(k, body):
        @pl.loop(0, 2)
        def _(way):
            blk = low + k + (1 - 2 * k) * way
            pl.when(jnp.logical_and(blk >= 0, blk < n))(lambda: body(blk))

    summed, crossing, closing = [], [], []

    def drain():
        if closing:
            k, j = closing.pop()
            reached(k, lambda blk: store(blk, j))
        if crossing:
            k, j = crossing.pop()
            reached(k, lambda blk: finish(blk, j))
            closing.append((k, j))
        if summed:
            k, j = summed.pop()
            reached(k, lambda blk: add_line(blk, j))
            crossing.append((k, j))

    def advance(k, j):
        drain()
        run(k, lambda blk: add_pair(blk, j))
        if k > 0:
            summed.append((k, j))

    def run(k, body):
        if k == 0:
            body(z)
        else:
            sides(k, lambda blk, way: body(blk))

    def middle():
        @pl.loop(0, 2 * tokens // step)
        def _(i):
            at = pl.ds(pl.multiple_of(i * step, step), step)
            value = gate[at, :]
            hidden[at, :] = (value / (1.0 + jnp.exp(-value)) * up[at, :]).astype(BF16)

        for j in range(CHUNKS):
            locals_[2 + j].wait()
            make_part(z, j)
            advance(0, j)

    token_move(t, pair, 0, True).wait_recv()
    for i, one in enumerate(others):
        token_move(t, one, 1 + i, False).start()

    def prepare():
        for d in (1, 2, 3):
            token_move(lax.rem(t + d, 4), mate, 0, False).wait_recv()
        norm(tokp, tokens)
        for u in (0, 1):
            locals_[u].wait()
            add_dot(u, z, first=True)

    events = [(u, k) for k in range(1, n) for u in (0, 1)]
    last_row = len(events)
    events += [(u, k) for k in range(1, n) for u in D_UNITS]
    for i in range(len(events) + LAG):
        if i < len(events):
            u, k = events[i]
            forward(u, k)
            if u == 1:
                pl.when(jnp.logical_and(n - 1 - z == k, z > 0))(lambda: send_own(D_UNITS, 0))
                pl.when(jnp.logical_and(z == k, z < n - 1))(lambda: send_own(D_UNITS, 1))
        if i == 0:
            prepare()
        if i >= LAG:
            use(*events[i - LAG])
            if i - LAG == last_row - 1:
                middle()
    for _ in range(3):
        drain()

    token_move(t, pair, 0, True).wait_send()
    for i, one in enumerate(others):
        token_move(t, one, 1 + i, False).wait_send()
    for u in range(2 + CHUNKS):
        for p in range(3):
            for way in (0, 1):
                pl.when(passes(p, jnp.int32(way)))(lambda: along(u, z, p, way, True).wait_send())
        for k in range(1, n):
            def sent(blk, way):
                for p in range(3):
                    pl.when(jnp.logical_and(arrives(p, way), passes(p, way)))(
                        lambda: along(u, blk, p, way).wait_send())
                swap(u, blk, 0, y).wait_send()
                pl.when(has_mid)(lambda: swap(u, blk, 1, y).wait_send())

            sides(k, sent)

    @pl.loop(0, n)
    def _(blk):
        for j in range(CHUNKS):
            to_mate(blk, j).wait_send()
            to_pair(blk, j).wait_send()
            to_across(blk, j).wait_send()
            give(blk, j, c).wait_send()
            write(blk, j).wait()


def fused(n, tokens, norm_gain, gate_weight, up_weight, down_weight):
    rows, width = tokens.shape
    depth, units = gate_weight.shape
    cols = down_weight.shape[1] // CHUNKS
    held = (units + 128) // 2
    dma = pltpu.SemaphoreType.DMA
    grid_of = (n, CHUNKS)
    hbm = pl.BlockSpec(memory_space=pl.ANY)
    vmem = pl.BlockSpec(memory_space=pltpu.VMEM)
    return pl.pallas_call(
        functools.partial(kernel, n),
        out_shape=jax.ShapeDtypeStruct((rows, width), BF16),
        in_specs=[vmem, vmem, hbm, hbm, hbm],
        out_specs=hbm,
        scratch_shapes=[
            pltpu.VMEM((rows, width), BF16),
            pltpu.VMEM((2 * rows, width), BF16),
            pltpu.VMEM((n, depth, units), BF16),
            pltpu.VMEM((n, depth, units), BF16),
            pltpu.VMEM((n, CHUNKS, units, cols), BF16),
            pltpu.VMEM((2 * rows, held), F32),
            pltpu.VMEM((2 * rows, held), F32),
            pltpu.VMEM((2 * rows, held), BF16),
            pltpu.VMEM((n, CHUNKS, 2, 2, rows // 2, cols), BF16),
            pltpu.VMEM((n, CHUNKS, 2, rows // 2, cols), BF16),
            pltpu.VMEM((n, CHUNKS, 2, rows // 2, cols), BF16),
            pltpu.VMEM((n, CHUNKS, rows // 2, cols), BF16),
            pltpu.VMEM((n, CHUNKS, rows // 2, cols), BF16),
            pltpu.VMEM((n, CHUNKS, rows // 2, cols), BF16),
            pltpu.VMEM((rows, width), BF16),
            dma((2 + CHUNKS,)),
            dma((2 + CHUNKS, n, 3, 2)),
            dma((2 + CHUNKS, n, 3)),
            dma((2 + CHUNKS, n, 2)),
            dma((2 + CHUNKS, n, 2)),
            dma((4,)),
            dma((4,)),
        ] + [dma(grid_of) for _ in range(9)],
        compiler_params=pltpu.CompilerParams(
            collective_id=0, has_side_effects=True, vmem_limit_bytes=60 * 2**20
        ),
    )(tokens, norm_gain.reshape(1, width), gate_weight, up_weight, down_weight)


def solution(mesh):
    n = mesh.shape["fs"]
    small = mesh.shape["rep"] == 2 and mesh.shape["tp"] == 4 and n == 4
    body = functools.partial(fused, n) if small else plain
    in_specs = (P(("rep", "fs"), None), P(), P("fs", "tp"), P("fs", "tp"), P("tp", "fs"))
    out_specs = P(("rep", "fs"), None)
    return jax.shard_map(
        body, mesh=mesh, in_specs=in_specs, out_specs=out_specs, check_vma=False
    )
```
